32 devices in a mesh: grp: 2 (over y), sp: 4 (over z), tp: 4 (over x, core).
Axes of the slice: x: 2, y: 2, z: 4, core: 2. Of those that a mesh axis runs over, the one named last changes fastest.
Arguments:
- latent: bfloat16 [4096, 4096], P(('grp', 'sp'), 'tp'), parts along dimension 0, may hold values from -42 to 42
- context: bfloat16 [2048, 4096], P(('grp', 'sp'), 'tp'), parts along dimension 0, may hold values from -42 to 42
- conditions: float32 [4, 4096], P('grp', 'sp'), parts along dimension 0, may hold values from -6 to 6
- mod_weight: bfloat16 [4096, 3, 4096], P('sp', None, 'tp'), may hold values from -0.09375 to 0.09375
- norm_gain: float32 [4096], P('tp'), may hold values from 0.1 to 1.9
- w_query: bfloat16 [4096, 2048], P(None, 'tp'), may hold values from -0.09375 to 0.09375
- w_key: bfloat16 [4096, 2048], P(None, 'tp'), may hold values from -0.09375 to 0.09375
- w_value: bfloat16 [4096, 2048], P(None, 'tp'), may hold values from -0.09375 to 0.09375
- query_gain: float32 [64], replicated, may hold values from 1 to 14
- key_gain: float32 [64], replicated, may hold values from 1 to 14
- lambdas: float32 [16], P('tp'), may hold values from 0.3 to 0.8
- out_gain: float32 [128], replicated, may hold values from 0.1 to 1.9
- w_out: bfloat16 [2048, 4096], P(None, 'tp'), may hold values from -0.125 to 0.125
Outputs:
- updated: bfloat16 [4096, 4096], P(('grp', 'sp'), 'tp'), parts along dimension 0
The draws below stay inside these ranges and needn't reach their ends.
There are 2 independent parts, one for each index of `grp`. The reference program is written for one: setup_inputs(seed, part) draws one part's arguments, and reference() takes and returns one part's arrays. A program takes and returns all parts, laid end to end along the dimension named above; an argument that names none is the same for every part. Nothing has to cross between parts.
All inputs are finite; a program needn't handle non-finite values.
Results may differ from the reference program's by a relative error of at most 0.0076.
Values may be sent and summed in bfloat16 or wider, within the bound.
A program may use at most 128 MiB of HBM per device.

```python
import math
import jax
import jax.numpy as jnp
from jax import lax

D = 4096
HEADS = 16
DK = 64
DV = 128
GRID_W = 64
CTX = 1024
LAT = 2048


def rising_rows(key, row_count):
    column = jnp.arange(D, dtype=jnp.float32)
    base = jnp.clip(jax.random.normal(key, (row_count, D), jnp.float32), -6.0, 6.0)
    return base * (1.0 + 2.0 * column / (D - 1))


def spiked_gains(key, which):
    own_key = jax.random.fold_in(key, which)
    return jax.random.uniform(own_key, (DK,), jnp.float32, 1.1, 1.5)


def draw_latent(key, part):
    return rising_rows(jax.random.fold_in(key, 21), LAT).astype(jnp.bfloat16)


def draw_context(key, part):
    return rising_rows(jax.random.fold_in(key, 22), CTX).astype(jnp.bfloat16)


def draw_query_gain(key, part):
    return spiked_gains(key, 1)


def draw_key_gain(key, part):
    return spiked_gains(key, 2)


def shard_levels(key, extent, pieces, smallest, high):
    loudness = 1.0
    for dim, parts in pieces:
        heights = jax.random.uniform(jax.random.fold_in(jax.random.fold_in(key, 6), dim), (parts,), jnp.float32, smallest / len(pieces), high / len(pieces))
        loudness = loudness * jnp.repeat(jnp.exp(heights), extent[dim] // parts).reshape((-1,) + (1,) * (len(extent) - 1 - dim))
    return loudness


def bell_draw(key, dims, deviation, most, shards=(), kind=jnp.bfloat16):
    result = deviation * jax.random.normal(key, dims, jnp.float32)
    if shards:
        result = result * shard_levels(key, dims, shards, -0.22, 0.18)
    return jnp.clip(result, -most, most).astype(kind)


def setup_inputs(seed: int = 0, part: int = 0) -> dict:
    keys = jax.random.split(jax.random.key(seed), 14)
    own_keys = jax.random.split(jax.random.fold_in(keys[13], part), 14)
    latent = draw_latent(jax.random.fold_in(jax.random.fold_in(keys[13], part), 71), part)
    context = draw_context(jax.random.fold_in(jax.random.fold_in(keys[13], part), 71), part)
    conditions = bell_draw(own_keys[2], (2, D), 1.0, 6.0, ((1, 4),), jnp.float32)
    mod_weight = bell_draw(keys[3], (D, 3, D), D ** -0.5, 0.09375, ((0, 4), (2, 4)))
    norm_gain = jnp.clip(1.0 + 0.18 * jax.random.normal(keys[4], (D,), jnp.float32), 0.1, 1.9)
    w_query = bell_draw(keys[5], (D, HEADS * 2 * DK), D ** -0.5, 0.09375, ((1, 4),))
    w_key = bell_draw(keys[6], (D, HEADS * 2 * DK), D ** -0.5, 0.09375, ((1, 4),))
    w_value = bell_draw(keys[7], (D, HEADS * DV), D ** -0.5, 0.09375, ((1, 4),))
    query_gain = draw_query_gain(jax.random.fold_in(keys[13], 71), part)
    key_gain = draw_key_gain(jax.random.fold_in(keys[13], 71), part)
    lambdas = jnp.clip(0.3 + 0.5 * jax.random.uniform(keys[10], (HEADS,), jnp.float32) ** shard_levels(keys[10], (HEADS,), ((0, 4),), -0.2, 0.2), 0.3, 0.8)
    out_gain = jnp.clip(1.0 + 0.18 * jax.random.normal(keys[11], (DV,), jnp.float32), 0.1, 1.9)
    w_out = bell_draw(keys[12], (HEADS * DV, D), (HEADS * DV) ** -0.5, 0.125, ((1, 4),))
    return {"latent": latent, "context": context, "conditions": conditions, "mod_weight": mod_weight, "norm_gain": norm_gain, "w_query": w_query, "w_key": w_key, "w_value": w_value, "query_gain": query_gain, "key_gain": key_gain, "lambdas": lambdas, "out_gain": out_gain, "w_out": w_out}


epsilon = 1e-06

def turn_half(halves, angles):
    quarter = halves.shape[-1] // 2
    cosine = jnp.cos(angles)[:, None, None, :]
    sine_part = jnp.sin(angles)[:, None, None, :]
    first_part = halves[..., :quarter]
    second = halves[..., quarter:]
    return jnp.concatenate([first_part * cosine - second * sine_part, first_part * sine_part + second * cosine], axis=-1)

def rotate(features, positions):
    half_width = features.shape[-1] // 2
    quarter = half_width // 2
    inverse = 10000.0 ** (-2.0 * jnp.arange(quarter, dtype=jnp.float32) / half_width)
    grid_row = (positions // GRID_W).astype(jnp.float32)
    grid_column = (positions % GRID_W).astype(jnp.float32)
    return jnp.concatenate([turn_half(features[..., :half_width], grid_row[:, None] * inverse), turn_half(features[..., half_width:], grid_column[:, None] * inverse)], axis=-1)

def head_norm(features, gain_row):
    return features * lax.rsqrt(lax.optimization_barrier(jnp.mean(features * features, axis=-1, keepdims=True)) + epsilon) * gain_row

def modulate(rows_in, gain_row, shift_row, scale_row):
    floats = rows_in.astype(jnp.float32)
    factor = lax.rsqrt(lax.optimization_barrier(jnp.mean(floats * floats, axis=1, keepdims=True)) + epsilon)
    return (floats * factor * gain_row * (1.0 + scale_row) + shift_row).astype(jnp.bfloat16)

def reference(latent, context, conditions, mod_weight, norm_gain, w_query, w_key, w_value, query_gain, key_gain, lambdas, out_gain, w_out):
    activated = jax.nn.silu(conditions).astype(jnp.bfloat16)
    modulation = jnp.dot(activated, mod_weight.reshape(D, 3 * D), preferred_element_type=jnp.float32).reshape(2, 3, D)
    hidden = modulate(latent, norm_gain, modulation[0, 0], modulation[0, 1])
    hidden_ctx = modulate(context, norm_gain, modulation[1, 0], modulation[1, 1])
    positions = jnp.arange(LAT, dtype=jnp.int32)
    query_raw = jnp.dot(hidden, w_query, preferred_element_type=jnp.float32).reshape(LAT, HEADS, 2, DK)
    key_raw = jnp.dot(hidden, w_key, preferred_element_type=jnp.float32).reshape(LAT, HEADS, 2, DK)
    ctx_key_raw = jnp.dot(hidden_ctx, w_key, preferred_element_type=jnp.float32).reshape(CTX, HEADS, 2, DK)
    queries = rotate(head_norm(query_raw, query_gain), positions).astype(jnp.bfloat16)
    lat_keys = rotate(head_norm(key_raw, key_gain), positions).astype(jnp.bfloat16)
    ctx_keys = head_norm(ctx_key_raw, key_gain).astype(jnp.bfloat16)
    lat_values = jnp.dot(hidden, w_value, preferred_element_type=jnp.float32).astype(jnp.bfloat16).reshape(LAT, HEADS, DV)
    ctx_values = jnp.dot(hidden_ctx, w_value, preferred_element_type=jnp.float32).astype(jnp.bfloat16).reshape(CTX, HEADS, DV)
    all_keys = jnp.concatenate([ctx_keys, lat_keys], axis=0)
    all_values = jnp.concatenate([ctx_values, lat_values], axis=0)
    block_rows = math.gcd(LAT, 512)
    scaling = DK ** (-0.5)

    def one_head(head_index):
        head_keys = lax.dynamic_index_in_dim(all_keys, head_index, 1, False).astype(jnp.float32)
        head_values = lax.dynamic_index_in_dim(all_values, head_index, 1, False).astype(jnp.float32)
        head_queries = lax.dynamic_index_in_dim(queries, head_index, 1, False).astype(jnp.float32)
        head_queries = head_queries.reshape(LAT // block_rows, block_rows, 2, DK)
        weight_lambda = lax.dynamic_index_in_dim(lambdas, head_index, 0, False)

        def one_block(query_block):
            scores = jnp.einsum('qmd,kmd->qmk', query_block, head_keys) * scaling
            row_peak = lax.optimization_barrier(jnp.max(scores, axis=-1, keepdims=True))
            exponent = jnp.exp(scores - row_peak)
            row_sums = lax.optimization_barrier(jnp.sum(exponent, axis=-1))
            weights = lax.optimization_barrier(exponent.astype(jnp.bfloat16)).astype(jnp.float32)
            blended = jnp.einsum('qmk,kv->qmv', weights, head_values)
            attended = blended[:, 0] / row_sums[:, 0, None] - weight_lambda * blended[:, 1] / row_sums[:, 1, None]
            return head_norm(attended, out_gain)
        return lax.map(one_block, head_queries).reshape(LAT, DV)
    outputs = lax.map(one_head, jnp.arange(HEADS, dtype=jnp.int32))
    head_out = jnp.transpose(outputs, (1, 0, 2)).reshape(LAT, HEADS * DV).astype(jnp.bfloat16)
    mixed_rows = jnp.dot(head_out, w_out, preferred_element_type=jnp.float32)
    return (latent.astype(jnp.float32) + modulation[0, 2] * mixed_rows).astype(jnp.bfloat16)
```

```python
import functools
import math

import jax
import jax.numpy as jnp
import numpy as np
from jax import lax
from jax.experimental import pallas as pl
from jax.experimental.pallas import tpu as pltpu
from jax.sharding import PartitionSpec as P

DK = 64
DV = 128
GRID_W = 64


epsilon = 1e-06


def turn_half(halves, angles):
    quarter = halves.shape[-1] // 2
    cosine = jnp.cos(angles)[:, None, None, :]
    sine_part = jnp.sin(angles)[:, None, None, :]
    first_part = halves[..., :quarter]
    second = halves[..., quarter:]
    return jnp.concatenate(
        [first_part * cosine - second * sine_part, first_part * sine_part + second * cosine],
        axis=-1,
    )


def rotate(features, positions):
    half_width = features.shape[-1] // 2
    quarter = half_width // 2
    inverse = 10000.0 ** (-2.0 * jnp.arange(quarter, dtype=jnp.float32) / half_width)
    grid_row = (positions // GRID_W).astype(jnp.float32)
    grid_column = (positions % GRID_W).astype(jnp.float32)
    return jnp.concatenate(
        [
            turn_half(features[..., :half_width], grid_row[:, None] * inverse),
            turn_half(features[..., half_width:], grid_column[:, None] * inverse),
        ],
        axis=-1,
    )


def head_norm(features, gain_row):
    return (
        features
        * lax.rsqrt(jnp.mean(features * features, axis=-1, keepdims=True) + epsilon)
        * gain_row
    )


def modulate(rows_in, gain_row, shift_row, scale_row):
    floats = rows_in.astype(jnp.float32)
    factor = lax.rsqrt(jnp.mean(floats * floats, axis=1, keepdims=True) + epsilon)
    return (floats * factor * gain_row * (1.0 + scale_row) + shift_row).astype(jnp.bfloat16)


def plain(
    latent,
    context,
    conditions,
    mod_weight,
    norm_gain,
    w_query,
    w_key,
    w_value,
    query_gain,
    key_gain,
    lambdas,
    out_gain,
    w_out,
):
    tok_rows = latent.shape[0]
    ctx_rows = context.shape[0]
    columns = latent.shape[1]
    heads_here = lambdas.shape[0]
    in_rows = mod_weight.shape[0]
    activated = jax.nn.silu(conditions).astype(jnp.bfloat16)
    partial_mod = jnp.dot(
        activated, mod_weight.reshape(in_rows, 3 * columns), preferred_element_type=jnp.float32
    ).reshape(2, 3, columns)
    modulation = lax.psum(partial_mod, "sp")
    lat_floats = latent.astype(jnp.float32)
    full_gain, full_pairs = (
        lax.all_gather(norm_gain, "tp", axis=0, tiled=True),
        lax.all_gather(modulation[:, :2], "tp", axis=2, tiled=True),
    )
    whole_lat, whole_ctx = (
        lax.all_gather(latent, "tp", axis=1, tiled=True),
        lax.all_gather(context, "tp", axis=1, tiled=True),
    )
    hidden = modulate(whole_lat, full_gain, full_pairs[0, 0], full_pairs[0, 1])
    hidden_ctx = modulate(whole_ctx, full_gain, full_pairs[1, 0], full_pairs[1, 1])
    query_raw = jnp.dot(hidden, w_query, preferred_element_type=jnp.float32)
    key_raw = jnp.dot(hidden, w_key, preferred_element_type=jnp.float32)
    value_raw = jnp.dot(hidden, w_value, preferred_element_type=jnp.float32)
    ctx_key_raw = jnp.dot(hidden_ctx, w_key, preferred_element_type=jnp.float32)
    ctx_value_raw = jnp.dot(hidden_ctx, w_value, preferred_element_type=jnp.float32)
    positions = lax.axis_index("sp") * tok_rows + jnp.arange(tok_rows, dtype=jnp.int32)
    queries = rotate(
        head_norm(query_raw.reshape(tok_rows, heads_here, 2, DK), query_gain), positions
    ).astype(jnp.bfloat16)
    lat_keys = (
        rotate(head_norm(key_raw.reshape(tok_rows, heads_here, 2, DK), key_gain), positions)
        .astype(jnp.bfloat16)
        .reshape(tok_rows, heads_here * 2 * DK)
    )
    lat_values = value_raw.astype(jnp.bfloat16)
    ctx_keys = (
        head_norm(ctx_key_raw.reshape(ctx_rows, heads_here, 2, DK), key_gain)
        .astype(jnp.bfloat16)
        .reshape(ctx_rows, heads_here * 2 * DK)
    )
    ctx_values = ctx_value_raw.astype(jnp.bfloat16)
    scaling = DK ** (-0.5)

    def absorb(carried, key_rows, value_rows):
        key_count = key_rows.shape[0]
        key_block = key_rows.reshape(key_count, heads_here, 2, DK)
        value_block = value_rows.reshape(key_count, heads_here, DV)
        running_max, totals, weighted = carried
        scores = (
            jnp.einsum("qhmd,khmd->qhmk", queries, key_block, preferred_element_type=jnp.float32)
            * scaling
        )
        new_max = jnp.maximum(running_max, jnp.max(scores, axis=-1))
        rescale = jnp.exp(running_max - new_max)
        exponent = jnp.exp(scores - new_max[..., None])
        totals = totals * rescale + jnp.sum(exponent, axis=-1)
        weighted = weighted * rescale[..., None] + jnp.einsum(
            "qhmk,khv->qhmv",
            exponent.astype(jnp.bfloat16),
            value_block,
            preferred_element_type=jnp.float32,
        )
        return (new_max, totals, weighted)

    def absorb_rows(carried, key_rows, value_rows):
        key_count = key_rows.shape[0]
        block_rows = math.gcd(key_count, 512)

        def visit_block(block_index, partial_value):
            first_row = block_index * block_rows
            return absorb(
                partial_value,
                lax.dynamic_slice_in_dim(key_rows, first_row, block_rows, 0),
                lax.dynamic_slice_in_dim(value_rows, first_row, block_rows, 0),
            )

        return lax.fori_loop(0, key_count // block_rows, visit_block, carried)

    initial_state = (
        jnp.full((tok_rows, heads_here, 2), -1e30, jnp.float32),
        jnp.zeros((tok_rows, heads_here, 2), jnp.float32),
        jnp.zeros((tok_rows, heads_here, 2, DV), jnp.float32),
    )
    every_ctx_keys, every_ctx_values = (
        lax.all_gather(ctx_keys, "sp", axis=0, tiled=True),
        lax.all_gather(ctx_values, "sp", axis=0, tiled=True),
    )
    carried = absorb_rows(initial_state, every_ctx_keys, every_ctx_values)
    carried = absorb_rows(
        carried,
        lax.all_gather(lat_keys, "sp", axis=0, tiled=True),
        lax.all_gather(lat_values, "sp", axis=0, tiled=True),
    )
    running_max, totals, weighted = carried
    attended = (
        weighted[:, :, 0] / totals[:, :, 0, None]
        - lambdas[None, :, None] * weighted[:, :, 1] / totals[:, :, 1, None]
    )
    head_out = head_norm(attended, out_gain).astype(jnp.bfloat16).reshape(tok_rows, heads_here * DV)
    mixed_rows = jnp.dot(
        lax.all_gather(head_out, "tp", axis=1, tiled=True),
        w_out,
        preferred_element_type=jnp.float32,
    )
    return (lat_floats + modulation[0, 2] * mixed_rows).astype(jnp.bfloat16)


MESH = pl.DeviceIdType.MESH
BF = jnp.bfloat16
F32 = jnp.float32
ROWS = 128


def flipped(position, bits, size):
    at = position
    step = 1
    while step < size:
        if bits & step:
            at = at + step - 2 * step * lax.rem(position // step, 2)
        step *= 2
    return at


def fused_kernel(
    sp, tp, lat, ctx, mw_h, wk_h, wv_h, wq_h, wo_h, cond_h, gain_h, qg_h, kg_h, rcos_h, rsin_h,
    ccos_h, csin_h, lam_h, og_h,
    out, X, MW, WK, WV, WQ, WO, cond, gain, qg, kg, rcos, rsin, ccos, csin, lambdas, og,
    PA, PG, CO, GT, H, SKV, SQ, RKV, RQ, SS, AC, PK, OS, HO,
    small_sem, loc_sem, m_sem, w_sem,
    xs, xr, ds, dr, fs, fr, ps, pr, ys, yr, cs, cr, ks, kr, qs_, qr, os_, or_, gs, gr, es, er, hs, hr,
):
    ms = lax.axis_index("sp")
    mt = lax.axis_index("tp")
    core = lax.rem(mt, 2)
    mate = mt + 1 - 2 * core
    far = lax.rem(mt + 2, tp)
    order = sorted(range(1, sp), key=lambda d: -d.bit_length())
    zp = [
        (1 - core) * flipped(ms, a, sp) + core * flipped(ms, b, sp)
        for a, b in zip(order, order[-1:] + order[:-1])
    ]
    tpn = [far, mate, lax.rem(mate + 2, tp)]
    cols = lat.shape[1]
    r = ROWS
    nc = ctx.shape[0] // r
    nl = lat.shape[0] // r

    barrier = pltpu.get_barrier_semaphore()
    for p in zp:
        pl.semaphore_signal(barrier, inc=1, device_id={"sp": p}, device_id_type=MESH)
    for p in tpn:
        pl.semaphore_signal(barrier, inc=1, device_id={"tp": p}, device_id_type=MESH)

    smalls = [
        pltpu.make_async_copy(a, b, small_sem.at[i])
        for i, (a, b) in enumerate(
            (
                (cond_h, cond), (gain_h, gain), (qg_h, qg), (kg_h, kg), (rcos_h, rcos),
                (rsin_h, rsin), (ccos_h, ccos), (csin_h, csin), (lam_h, lambdas), (og_h, og),
            )
        )
    ]
    for s in smalls:
        s.start()
    mods = [pltpu.make_async_copy(mw_h.at[j], MW.at[j], m_sem.at[j]) for j in range(3)]
    for m in mods:
        m.start()

    def source(c):
        return ctx.at[pl.ds(c * r, r)] if c < nc else lat.at[pl.ds((c - nc) * r, r)]

    def rows_of(c):
        return pl.ds(c * r if isinstance(c, int) else pl.multiple_of(c * r, r), r)

    locals_ = [
        pltpu.make_async_copy(ctx, X.at[mt, pl.ds(0, nc * r)], loc_sem.at[0]),
        pltpu.make_async_copy(lat, X.at[mt, pl.ds(nc * r, nl * r)], loc_sem.at[1]),
    ]
    for copy in locals_:
        copy.start()
    weights = [
        pltpu.make_async_copy(a, b, w_sem.at[i])
        for i, (a, b) in enumerate(((wk_h, WK), (wv_h, WV), (wq_h, WQ), (wo_h, WO)))
    ]
    for w in weights:
        w.start()
    RKV[:, :, 2 * DV:3 * DV] = jnp.ones((nc + nl, sp * r, DV), BF)
    with jax.named_scope("barrier"):
        pl.semaphore_wait(barrier, (sp - 1) + (tp - 1))

    def remote(src, dst, ssem, rsem, where):
        return pltpu.make_async_remote_copy(
            src_ref=src, dst_ref=dst, send_sem=ssem, recv_sem=rsem,
            device_id=where, device_id_type=MESH,
        )

    def x_send(c, src=None):
        ref = X.at[mt, rows_of(c)]
        return remote(ref if src is None else src, ref, xs.at[c], xr.at[c], {"tp": far})

    def d_send(c, src=None):
        ref = X.at[mt, rows_of(c)]
        return remote(ref if src is None else src, ref, ds.at[c], dr.at[c], {"tp": mate})

    def f_send(c):
        ref = X.at[far, rows_of(c)]
        return remote(ref, ref, fs.at[c], fr.at[c], {"tp": mate})

    def p_send(d):
        return remote(PA.at[ms], PA.at[ms], ps.at[d], pr.at[d], {"sp": zp[d]})

    def y_send(d):
        return remote(PG.at[ms], PG.at[ms], ys.at[d], yr.at[d], {"sp": zp[d]})

    def c_send(d):
        return remote(CO.at[mt], CO.at[mt], cs.at[d], cr.at[d], {"tp": tpn[d]})

    x_send(0, source(0)).start()
    for c in range(nc + nl):
        d_send(c, source(c)).start()

    with jax.named_scope("mod"):
        smalls[0].wait()
        value = cond[...]
        act = value / (1.0 + jnp.exp(-value))
        act = jnp.concatenate([act, jnp.zeros((14, act.shape[1]), F32)], axis=0).astype(BF)
        mods[0].wait()
        shifts = jnp.dot(act, MW[0], preferred_element_type=F32)
        mods[1].wait()
        scales = jnp.dot(act, MW[1], preferred_element_type=F32)
        PA[ms] = jnp.concatenate([shifts[0:1], scales[0:1], shifts[1:2], scales[1:2]], axis=0)
        for d in range(sp - 1):
            p_send(d).start()
        mods[2].wait()
        PG[ms] = jnp.dot(act, MW[2], preferred_element_type=F32)[0:1]
        for d in range(sp - 1):
            y_send(d).start()
        for s in smalls[1:]:
            s.wait()
    with jax.named_scope("pwait"):
        for d in range(sp - 1):
            p_send(d).wait()
    total = PA[0]
    for s in range(1, sp):
        total = total + PA[s]
    CO[mt] = jnp.concatenate(
        [
            gain[...] * (1.0 + total[1:2]), total[0:1],
            gain[...] * (1.0 + total[3:4]), total[2:3],
        ],
        axis=0,
    )
    for d in range(tp - 1):
        c_send(d).start()
    for c in range(1, nc + nl):
        x_send(c, source(c)).start()

    lane = lax.broadcasted_iota(jnp.int32, (2 * r, 2 * DK), 1)
    low = lax.rem(lane, DK // 2) < DK // 4
    by_row = lax.rem(lane[:GRID_W], DK) < DK // 2
    bd_row = lax.broadcasted_iota(jnp.int32, (2 * DK, 2 * DK), 0) < DK
    bd_col = lax.broadcasted_iota(jnp.int32, (2 * DK, 2 * DK), 1) < DK
    ones_bd = jnp.where(bd_row == bd_col, 1.0, 0.0).astype(BF)

    def swapped(v):
        where = low[:v.shape[0]]
        return jnp.where(where, pltpu.roll(v, 2 * DK - DK // 4, 1), pltpu.roll(v, DK // 4, 1))

    def gains(ref, scale):
        g = jnp.concatenate([ref[...], ref[...]], axis=1) * scale
        return g, swapped(jnp.broadcast_to(g, (8, 2 * DK)))[0:1]

    q_gain, q_swap = gains(qg, DK ** (-0.5) * math.log2(math.e))
    k_gain, k_swap = gains(kg, 1.0)
    heads_lane = lax.broadcasted_iota(jnp.int32, lambdas.shape, 1)
    lam = jnp.sum(jnp.where(heads_lane == ms, lambdas[...], 0.0), axis=1, keepdims=True)

    def table(row_ref, col_ref, block):
        start = ms * (nl * r // GRID_W) + block * (r // GRID_W)
        return jnp.concatenate(
            [
                jnp.where(by_row, row_ref[pl.ds(start + k, 1), :], col_ref[...])
                for k in range(r // GRID_W)
            ],
            axis=0,
        )

    def own(size=ROWS):
        return pl.ds(pl.multiple_of(ms * size, size), size)

    def k_send(c, d):
        return remote(
            SKV.at[c, zp[d]], RKV.at[c, own(), pl.ds(0, 2 * DV)], ks.at[c, d], kr.at[c, d],
            {"sp": zp[d]},
        )

    def q_send(block, d):
        return remote(
            SQ.at[block, zp[d]], RQ.at[block, own()], qs_.at[block, d], qr.at[block, d],
            {"sp": zp[d]},
        )

    def normed(v):
        square = (v * v).astype(BF)
        mean = jnp.dot(square, ones_bd, preferred_element_type=F32)
        return v * lax.rsqrt(mean * (1.0 / DK) + epsilon)

    def turned(v, ctab, stab):
        w = normed(v)
        return (w * ctab + swapped(w) * stab).astype(BF)

    def arrive(c, first_row):
        rows = rows_of(c)
        with jax.named_scope("xwait"):
            x_send(c).wait_recv()
            f_send(c).start()
            d_send(c).wait_recv()
            f_send(c).wait_recv()
        with jax.named_scope("norm"):
            square = jnp.zeros((r, 128), F32)
            for t in range(tp):
                f = X[t, rows, :].astype(F32)
                f = f * f
                for m in range(cols // 128):
                    square = square + f[:, m * 128:(m + 1) * 128]
            ss = jnp.sum(square, axis=1, keepdims=True)
            factor = lax.rsqrt(ss * (1.0 / (tp * cols)) + epsilon)
            for t in range(tp):
                f = X[t, rows, :].astype(F32)
                H[:, t * cols:(t + 1) * cols] = (
                    f * factor * CO[t, first_row:first_row + 1] + CO[t, first_row + 1:first_row + 2]
                ).astype(BF)

    def values(c):
        raw = jnp.dot(H[...], WV[...], preferred_element_type=F32)
        for z in range(sp):
            SKV[c, z, :, DV:2 * DV] = raw[:, z * DV:(z + 1) * DV].astype(BF)
        for d in range(sp - 1):
            k_send(c, d).start()
        RKV[c, own(), 0:2 * DV] = SKV[c, ms]

    def context_chunk(c, carry):
        arrive(c, 2)
        with jax.named_scope("kv"):
            raw = jnp.dot(H[...], WK[...], preferred_element_type=F32)
            for z in range(sp):
                piece = raw[:, z * DV:(z + 1) * DV]
                SKV[c, z, :, 0:DV] = (normed(piece) * k_gain).astype(BF)
            values(c)
        return carry

    def latent_chunk(block, carry):
        c = nc + block
        arrive(c, 0)
        with jax.named_scope("qkv"):
            cosine, sine = table(rcos, ccos, block), table(rsin, csin, block)
            qc, qs = cosine * q_gain, sine * q_swap
            kc, ks_ = cosine * k_gain, sine * k_swap
            raw = jnp.dot(H[...], WK[...], preferred_element_type=F32)
            for z in range(sp):
                SKV[c, z, :, 0:DV] = turned(raw[:, z * DV:(z + 1) * DV], kc, ks_)
            values(c)
            raw = jnp.dot(H[...], WQ[...], preferred_element_type=F32)
            for z in range(sp):
                SQ[block, z] = turned(raw[:, z * DV:(z + 1) * DV], qc, qs)
            for d in range(sp - 1):
                q_send(block, d).start()
            RQ[block, own()] = SQ[block, ms]
        return carry

    for copy in locals_:
        copy.wait()
    with jax.named_scope("cwait"):
        for d in range(tp - 1):
            c_send(d).wait_recv()
        weights[0].wait()
        weights[1].wait()
    lax.fori_loop(0, nc, context_chunk, 0)
    weights[2].wait()
    lax.fori_loop(0, nl, latent_chunk, 0)

    half = sp * r // 2
    first = lane < DK

    def merge(old, new):
        peak = jnp.maximum(old[0], new[0])
        return peak, old[1] * jnp.exp2(old[0] - peak) + new[1] * jnp.exp2(new[0] - peak)

    def stacked(block, side):
        q = RQ[block, side * half:(side + 1) * half, :]
        zero = jnp.zeros_like(q)
        where = first[:half]
        return jnp.concatenate([jnp.where(where, q, zero), jnp.where(where, zero, q)], axis=0)

    def attend(block, groups, states):
        queries = [stacked(block, side) for side in range(2)]
        stages = [(side, g) for side in range(2) for g in groups]
        peaks = {}

        def keys(g, j, first_lane):
            return RKV[2 * g + j // 2, (j % 2) * half:(j % 2 + 1) * half, first_lane]

        def score(k, j):
            side, g = stages[k]
            s = lax.dot_general(
                queries[side], keys(g, j, slice(0, DV)), (((1,), (1,)), ((), ())),
                preferred_element_type=F32,
            )
            SS[(k % 3) * 4 + j] = s
            for m in range(half // 128):
                piece = s[:, m * 128:(m + 1) * 128]
                peaks[k] = piece if k not in peaks else jnp.maximum(peaks[k], piece)

        for j in range(4):
            score(0, j)
        for k, (side, g) in enumerate(stages):
            peak = jnp.max(peaks[k], axis=1, keepdims=True)
            acc = None
            for j in range(4):
                p = jnp.exp2(SS[(k % 3) * 4 + j] - peak).astype(BF)
                term = jnp.dot(p, keys(g, j, slice(DV, 3 * DV)), preferred_element_type=F32)
                acc = term if acc is None else acc + term
                if k + 1 < len(stages):
                    score(k + 1, j)
            new = (peak, acc)
            states[side] = new if states[side] is None else merge(states[side], new)
        return states

    def o_send(block, d):
        return remote(
            OS.at[block, pl.ds(pl.multiple_of(zp[d] * r, r), r)],
            HO.at[mt, block, :, own(DV)], os_.at[block, d], or_.at[block, d], {"sp": zp[d]},
        )

    def finish(block, states):
        for side in range(2):
            acc = states[side][1]
            o = acc[:, :DV] / acc[:, DV:]
            a = o[:half] - lam * o[half:]
            a = a * lax.rsqrt(jnp.mean(a * a, axis=1, keepdims=True) + epsilon) * og[...]
            OS[block, side * half:(side + 1) * half] = a.astype(BF)
        for d in range(sp - 1):
            o_send(block, d).start()
        HO[mt, block, :, own(DV)] = OS[block, own()]

    def keys_in(c):
        with jax.named_scope("kwait"):
            for d in range(sp - 1):
                k_send(c, d).wait_recv()

    def queries_in(block):
        with jax.named_scope("qwait"):
            for d in range(sp - 1):
                q_send(block, d).wait_recv()

    early = nl // 2
    for c in range(nc + early):
        keys_in(c)

    def ahead(block, carry):
        queries_in(block)
        for side, (peak, acc) in enumerate(attend(block, (0, 1), [None, None])):
            AC[block, side] = acc
            PK[block, side] = jnp.broadcast_to(peak, (2 * half, 128))
        return carry

    with jax.named_scope("ahead"):
        lax.fori_loop(0, early, ahead, 0)
    for c in range(nc + early, nc + nl):
        keys_in(c)

    def close(block, carry):
        states = [(PK[block, side][:, 0:1], AC[block, side]) for side in range(2)]
        finish(block, attend(block, (2,), states))
        return carry

    with jax.named_scope("close"):
        lax.fori_loop(0, early, close, 0)

    def whole(block, carry):
        queries_in(block)
        with jax.named_scope("whole"):
            finish(block, attend(block, (0, 1, 2), [None, None]))
        return carry

    lax.fori_loop(early, nl, whole, 0)
    last = nl - 1

    def g_send(block):
        ref = HO.at[mt, block]
        return remote(ref, ref, gs.at[block], gr.at[block], {"tp": far})

    def e_send(block):
        ref = HO.at[mt, block]
        return remote(ref, ref, es.at[block], er.at[block], {"tp": mate})

    def h_send(block):
        ref = HO.at[far, block]
        return remote(ref, ref, hs.at[block], hr.at[block], {"tp": mate})

    def relay(block):
        with jax.named_scope("owait"):
            for d in range(sp - 1):
                o_send(block, d).wait_recv()
        g_send(block).start()
        e_send(block).start()

    width = sp * DV

    def emit(block):
        with jax.named_scope("gwait"):
            g_send(block).wait_recv()
            h_send(block).start()
            e_send(block).wait_recv()
            h_send(block).wait_recv()
        with jax.named_scope("outmm"):
            mixed = jnp.zeros((r, cols), F32)
            for t in range(tp):
                mixed = mixed + jnp.dot(
                    HO[t, block], WO[t * width:(t + 1) * width, :], preferred_element_type=F32
                )
            residual = X[mt, rows_of(nc + block), :].astype(F32)
            out[rows_of(block), :] = (residual + GT[...] * mixed).astype(BF)

    weights[3].wait()
    for d in range(sp - 1):
        y_send(d).wait()
    gate = PG[0]
    for s in range(1, sp):
        gate = gate + PG[s]
    GT[...] = gate
    relay(0)

    def pipeline(block, carry):
        relay(block)
        emit(block - 1)
        return carry

    lax.fori_loop(1, nl, pipeline, 0)
    emit(last)
    with jax.named_scope("sends"):
        for d in range(tp - 1):
            c_send(d).wait_send()
        for c in range(nc + nl):
            x_send(c).wait_send()
            d_send(c).wait_send()
            f_send(c).wait_send()
            for d in range(sp - 1):
                k_send(c, d).wait_send()
        for block in range(nl):
            for d in range(sp - 1):
                q_send(block, d).wait_send()
                o_send(block, d).wait_send()
            g_send(block).wait_send()
            e_send(block).wait_send()
            h_send(block).wait_send()


def fused(
    sp, tp, latent, context, conditions, mod_weight, norm_gain, w_query, w_key, w_value,
    query_gain, key_gain, lambdas, out_gain, w_out,
):
    tok, cols = latent.shape
    n = context.shape[0]
    r = ROWS
    nc, nl = n // r, tok // r
    inverse = 10000.0 ** (-4.0 * np.arange(DK // 4) / DK)
    sign = np.where(np.arange(2 * DK) % (DK // 2) < DK // 4, -1.0, 1.0)

    def trig(count):
        angles = np.arange(count)[:, None] * np.tile(inverse, 8)[None]
        return (
            jnp.asarray(np.cos(angles).astype(np.float32)),
            jnp.asarray((np.sin(angles) * sign).astype(np.float32)),
        )

    rcos, rsin = trig(sp * tok // GRID_W)
    ccos, csin = trig(GRID_W)
    smalls = (
        conditions, norm_gain[None], query_gain[None], key_gain[None], rcos, rsin, ccos, csin,
        lambdas[None], out_gain[None],
    )
    any_ = pl.BlockSpec(memory_space=pl.ANY)
    dma = pltpu.SemaphoreType.DMA
    mod = jnp.transpose(mod_weight, (1, 0, 2))
    big = (mod, w_key, w_value, w_query, w_out)
    return pl.pallas_call(
        functools.partial(fused_kernel, sp, tp),
        out_shape=pltpu.VMEM((tok, cols), BF),
        in_specs=[any_] * (2 + len(big) + len(smalls)),
        out_specs=pl.BlockSpec(memory_space=pltpu.VMEM),
        scratch_shapes=[pltpu.VMEM((tp, n + tok, cols), BF)]
        + [pltpu.VMEM(a.shape, BF) for a in big]
        + [pltpu.VMEM(a.shape, F32) for a in smalls]
        + [
            pltpu.VMEM((sp, 4, cols), F32),
            pltpu.VMEM((sp, 1, cols), F32),
            pltpu.VMEM((tp, 4, cols), F32),
            pltpu.VMEM((1, cols), F32),
            pltpu.VMEM((r, tp * cols), BF),
            pltpu.VMEM((nc + nl, sp, r, 2 * DV), BF),
            pltpu.VMEM((nl, sp, r, DV), BF),
            pltpu.VMEM((nc + nl, sp * r, 3 * DV), BF),
            pltpu.VMEM((nl, sp * r, DV), BF),
            pltpu.VMEM((12, sp * r, sp * r // 2), F32),
            pltpu.VMEM((nl // 2, 2, sp * r, 2 * DV), F32),
            pltpu.VMEM((nl // 2, 2, sp * r, 128), F32),
            pltpu.VMEM((nl, sp * r, DV), BF),
            pltpu.VMEM((tp, nl, r, sp * DV), BF),
            dma((len(smalls),)), dma((2,)), dma((3,)), dma((4,)),
            dma((nc + nl,)), dma((nc + nl,)),
            dma((nc + nl,)), dma((nc + nl,)),
            dma((nc + nl,)), dma((nc + nl,)),
            dma((sp - 1,)), dma((sp - 1,)),
            dma((sp - 1,)), dma((sp - 1,)),
            dma((tp - 1,)), dma((tp - 1,)),
            dma((nc + nl, sp - 1)), dma((nc + nl, sp - 1)),
            dma((nl, sp - 1)), dma((nl, sp - 1)),
            dma((nl, sp - 1)), dma((nl, sp - 1)),
            dma((nl,)), dma((nl,)),
            dma((nl,)), dma((nl,)),
            dma((nl,)), dma((nl,)),
        ],
        compiler_params=pltpu.CompilerParams(
            collective_id=0, has_side_effects=True, vmem_limit_bytes=60 * 1024 * 1024
        ),
    )(latent, context, *big, *smalls)


def local(sp, tp, *arguments):
    latent, context, lambdas = arguments[0], arguments[1], arguments[10]
    fits = (
        lambdas.shape[0] == sp and sp == 4 and tp == 4
        and latent.shape[0] == 4 * ROWS and context.shape[0] == 2 * ROWS
        and latent.shape[1] % 128 == 0 and latent.shape[1] <= 1024
    )
    if fits:
        return fused(sp, tp, *arguments)
    return plain(*arguments)


def solution(mesh):
    in_specs = (
        P(("grp", "sp"), "tp"),
        P(("grp", "sp"), "tp"),
        P("grp", "sp"),
        P("sp", None, "tp"),
        P("tp"),
        P(None, "tp"),
        P(None, "tp"),
        P(None, "tp"),
        P(),
        P(),
        P("tp"),
        P(),
        P(None, "tp"),
    )
    out_specs = P(("grp", "sp"), "tp")
    body = functools.partial(local, mesh.shape["sp"], mesh.shape["tp"])
    return jax.shard_map(body, mesh=mesh, in_specs=in_specs, out_specs=out_specs, check_vma=False)
```
